32 devices in a mesh: sp: 8 (over z, x), tp: 4 (over y, core).
Axes of the slice: x: 2, y: 2, z: 4, core: 2. Of those that a mesh axis runs over, the one named last changes fastest.
Arguments:
- tokens: bfloat16 [4096, 2048], P(('sp', 'tp')), may hold values from -6 to 6
- norm_gain: float32 [2048], replicated, may hold values from 0.1 to 1.9
- rec_query: bfloat16 [2048, 1024], P(None, 'tp'), may hold values from -0.125 to 0.125
- fwd_gate: bfloat16 [2048, 1024], P(None, 'tp'), may hold values from -0.125 to 0.125
- bwd_gate: bfloat16 [2048, 1024], P(None, 'tp'), may hold values from -0.125 to 0.125
- rec_value: bfloat16 [2048, 1024], P(None, 'tp'), may hold values from -0.125 to 0.125
- gate_leak: float32 [2, 1024], P(None, 'tp'), may hold values from 0 to 0.08, as said below
- log_decay: float32 [2, 4096, 8], P(None, 'sp', 'tp'), may hold values from -2.2 to 0, as said below
- rec_gain: float32 [128], replicated, may hold values from 0.1 to 1.9
- att_query: bfloat16 [2048, 1024], P(None, 'tp'), as said below
- att_key: bfloat16 [2048, 1024], P(None, 'tp')
- att_value: bfloat16 [2048, 1024], P(None, 'tp'), may hold values from -0.125 to 0.125
- lambdas: float32 [8], P('tp'), may hold values from 0.3 to 0.8
- att_gain: float32 [128], replicated, may hold values from 0.1 to 1.9
- out_rec: bfloat16 [1024, 2048], replicated, may hold values from -0.125 to 0.125
- out_att: bfloat16 [1024, 2048], replicated, may hold values from -0.125 to 0.125
Outputs:
- layer_out: bfloat16 [4096, 2048], P(('sp', 'tp'))
The draws below stay inside these ranges and needn't reach their ends.
Inputs may be any that keep to these rules, and one draw needn't show every extreme that they name: `gate_leak`: positive, by direction and channel. `log_decay`: never positive. `att_query`: entries of order 2048 to the power -1/2.
All inputs are finite; a program needn't handle non-finite values.
Results may differ from the reference program's by a relative error of at most 0.011.
Values may be sent and summed in bfloat16 or wider, within the bound.
A program may use at most 128 MiB of HBM per device.

```python
import jax
import jax.numpy as jnp
from jax import lax

D = 2048
HR = 8
HK = 128
HV = 128
HA = 8
AK = 64
AV = 128
BLOCK = 64
TOK_DEV = 512
SEQ = 4096


def draw_gate_leak(key, part):
    pick_key, slow_key, fast_key = jax.random.split(jax.random.fold_in(key, 3), 3)
    slow_share = 0.5
    slow_heads = jax.random.uniform(pick_key, (2, HR, 1), jnp.float32) < slow_share
    slow_rates = jnp.exp(jax.random.uniform(slow_key, (2, HR, HK), jnp.float32, jnp.log(0.3), jnp.log(1.0))) / SEQ
    fast_rates = jnp.exp(jax.random.uniform(fast_key, (2, HR, HK), jnp.float32, jnp.log(0.03), jnp.log(0.08)))
    return jnp.where(slow_heads, slow_rates, fast_rates).reshape(2, HR * HK)


def draw_log_decay(key, part):
    rate_key, spot_key, depth_key = jax.random.split(jax.random.fold_in(key, 5), 3)
    low_rate = 0.3
    high_rate = 1.2
    block_count = SEQ // TOK_DEV
    rates = jnp.exp(jax.random.uniform(rate_key, (2, block_count, 1, HR), jnp.float32, jnp.log(low_rate), jnp.log(high_rate)))
    stable_baseline = jnp.broadcast_to(-rates / SEQ, (2, block_count, TOK_DEV, HR)).reshape(2, SEQ, HR)
    marked_locations = jax.random.randint(spot_key, (2, 3, 1, HR), 0, SEQ)
    layer_depth_list = jax.random.uniform(depth_key, (2, 3, 1, HR), jnp.float32, jnp.log(0.5), jnp.log(0.8))
    token_locations = jnp.arange(SEQ, dtype=jnp.int32)[None, None, :, None]
    spike_events = jnp.sum(jnp.where(token_locations == marked_locations, layer_depth_list, 0.0), axis=1)
    return stable_baseline + spike_events


def attention_pair(key):
    base_key, own_key = jax.random.split(jax.random.fold_in(key, 7), 2)
    columns = HA * 2 * AK
    query_table = jax.random.normal(base_key, (D, columns), jnp.float32) * (3.0 / D) ** 0.5
    key_table = jax.random.normal(own_key, (D, columns), jnp.float32) / D ** 0.5
    return (query_table, key_table)


def draw_att_query(key, part):
    return attention_pair(key)[0].astype(jnp.bfloat16)


def draw_att_key(key, part):
    return attention_pair(key)[1].astype(jnp.bfloat16)


def shard_levels(key, extent, pieces, low, largest):
    factor_of, own = 1.0, jax.random.fold_in(key, 6)
    for dim, blocks in pieces:
        draws = jnp.exp(jax.random.uniform(jax.random.fold_in(own, dim), (blocks,), jnp.float32, low / len(pieces), largest / len(pieces)))
        factor_of = factor_of * jnp.repeat(draws, extent[dim] // blocks).reshape([-1 if axis == dim else 1 for axis in range(len(extent))])
    return factor_of


def bell_draw(rng, extent, deviation, limit, pieces=(), kind=jnp.bfloat16):
    level = shard_levels(rng, extent, pieces, -0.22, 0.18) if pieces else 1.0
    result = jax.random.normal(rng, extent, jnp.float32) * deviation * level
    return jnp.minimum(jnp.maximum(result, -limit), limit).astype(kind)


def setup_inputs(seed: int = 0) -> dict:
    arg_keys = jax.random.split(jax.random.key(seed), 17)
    return {
        "tokens": bell_draw(arg_keys[0], (SEQ, D), 1.0, 6.0, ((0, 32),)),
        "norm_gain": jnp.clip(1.0 + 0.18 * jax.random.normal(arg_keys[1], (D,), jnp.float32), 0.1, 1.9),
        "rec_query": bell_draw(arg_keys[2], (D, HR * HK), D ** -0.5, 0.125, ((1, 4),)),
        "fwd_gate": bell_draw(arg_keys[3], (D, HR * HK), D ** -0.5, 0.125, ((1, 4),)),
        "bwd_gate": bell_draw(arg_keys[4], (D, HR * HK), D ** -0.5, 0.125, ((1, 4),)),
        "rec_value": bell_draw(arg_keys[5], (D, HR * HV), D ** -0.5, 0.125, ((1, 4),)),
        "gate_leak": draw_gate_leak(jax.random.fold_in(arg_keys[16], 71), 0),
        "log_decay": draw_log_decay(jax.random.fold_in(arg_keys[16], 71), 0),
        "rec_gain": jnp.clip(1.0 + 0.18 * jax.random.normal(arg_keys[8], (HV,), jnp.float32), 0.1, 1.9),
        "att_query": draw_att_query(jax.random.fold_in(arg_keys[16], 71), 0),
        "att_key": draw_att_key(jax.random.fold_in(arg_keys[16], 71), 0),
        "att_value": bell_draw(arg_keys[11], (D, HA * AV), D ** -0.5, 0.125, ((1, 4),)),
        "lambdas": jnp.clip(0.3 + 0.5 * jax.random.uniform(arg_keys[12], (HA,), jnp.float32) ** shard_levels(arg_keys[12], (HA,), ((0, 4),), -0.2, 0.2), 0.3, 0.8),
        "att_gain": jnp.clip(1.0 + 0.18 * jax.random.normal(arg_keys[13], (AV,), jnp.float32), 0.1, 1.9),
        "out_rec": bell_draw(arg_keys[14], (HR * HV, D), (HR * HV + HA * AV) ** -0.5, 0.125),
        "out_att": bell_draw(arg_keys[15], (HA * AV, D), (HR * HV + HA * AV) ** -0.5, 0.125),
    }


EPS = 1e-06
THETA = 500000.0
HIGHEST = lax.Precision.HIGHEST

def rms_scale(values, gain):
    return values * lax.rsqrt(lax.optimization_barrier(jnp.mean(values * values, axis=-1, keepdims=True)) + EPS) * gain

def block_recurrence(queries, keys_in, values, log_forget):
    head_count, length, key_width = queries.shape
    value_width = values.shape[-1]
    block_count = length // BLOCK
    block_shape = (head_count, block_count, BLOCK, key_width)
    query_blocks = queries.reshape(block_shape)
    key_blocks = keys_in.reshape(block_shape)
    value_blocks = values.reshape(head_count, block_count, BLOCK, value_width)
    cumulative = jnp.cumsum(log_forget.reshape(block_shape), axis=2)
    middle = cumulative[:, :, BLOCK // 2 - 1:BLOCK // 2]
    block_last = cumulative[:, :, BLOCK - 1:]
    scores = jnp.einsum('hntd,hnsd->hnts', query_blocks * jnp.exp(cumulative - middle), key_blocks * jnp.exp(middle - cumulative), precision=HIGHEST)
    causal_mask = jnp.arange(BLOCK)[:, None] >= jnp.arange(BLOCK)[None, :]
    scores = jnp.where(causal_mask, scores, 0.0)
    within_out = jnp.einsum('hnts,hnsv->hntv', scores, value_blocks, precision=HIGHEST)
    per_block_state = jnp.einsum('hnsd,hnsv->hndv', key_blocks * jnp.exp(block_last - cumulative), value_blocks, precision=HIGHEST)
    block_decay = jnp.exp(block_last[:, :, 0])

    def advance(running, inputs_now):
        factor, added_state = inputs_now
        return (factor[..., None] * running + added_state, running)
    initial = jnp.zeros((head_count, key_width, value_width), jnp.float32)
    end_state, before = lax.scan(advance, initial, (jnp.moveaxis(block_decay, 1, 0), jnp.moveaxis(per_block_state, 1, 0)))
    before = jnp.moveaxis(before, 0, 1)
    carried = jnp.einsum('hntd,hndv->hntv', query_blocks * jnp.exp(cumulative), before, precision=HIGHEST)
    return ((within_out + carried).reshape(head_count, length, value_width), end_state, cumulative)

def rotate(vectors, positions):
    half_width = AK // 2
    frequency = THETA ** (-(jnp.arange(half_width, dtype=jnp.float32) * 2.0 / AK))
    angles = positions[:, None] * frequency[None, :]
    cosine = jnp.cos(angles)[:, None, None, :]
    sines = jnp.sin(angles)[:, None, None, :]
    first_half = vectors[..., :half_width]
    second = vectors[..., half_width:]
    return jnp.concatenate([first_half * cosine - second * sines, second * cosine + first_half * sines], axis=-1)

def reference(tokens, norm_gain, rec_query, fwd_gate, bwd_gate, rec_value, gate_leak, log_decay, rec_gain, att_query, att_key, att_value, lambdas, att_gain, out_rec, out_att):
    normed = rms_scale(tokens.astype(jnp.float32), norm_gain).astype(jnp.bfloat16)

    def project(weight):
        return jnp.dot(normed, weight, preferred_element_type=jnp.float32).astype(jnp.bfloat16)

    def split_heads(table, width):
        return table.astype(jnp.float32).reshape(SEQ, -1, width).transpose(1, 0, 2)
    queries = jax.nn.silu(split_heads(project(rec_query), HK))
    values = split_heads(project(rec_value), HV)
    key_fwd = gate_leak[0].reshape(HR, 1, HK) * jax.nn.sigmoid(-split_heads(project(fwd_gate), HK))
    key_bwd = gate_leak[1].reshape(HR, 1, HK) * jax.nn.sigmoid(-split_heads(project(bwd_gate), HK))
    log_fwd = jnp.log1p(-key_fwd) + log_decay[0].T[:, :, None]
    log_bwd = jnp.log1p(-key_bwd) + log_decay[1].T[:, :, None]
    out_fwd = block_recurrence(queries, key_fwd, values, log_fwd)[0]
    flipped = block_recurrence(jnp.flip(queries, 1), jnp.flip(key_bwd, 1), jnp.flip(values, 1), jnp.flip(log_bwd, 1))[0]
    rec_rows = rms_scale(out_fwd + jnp.flip(flipped, 1), rec_gain)
    rec_rows = rec_rows.transpose(1, 0, 2).reshape(SEQ, HR * HV).astype(jnp.bfloat16)
    positions = jnp.arange(SEQ, dtype=jnp.int32).astype(jnp.float32)
    att_queries = (rotate(project(att_query).astype(jnp.float32).reshape(SEQ, HA, 2, AK), positions) * AK ** (-0.5)).astype(jnp.bfloat16)
    att_keys = rotate(project(att_key).astype(jnp.float32).reshape(SEQ, HA, 2, AK), positions).astype(jnp.bfloat16)
    att_values = project(att_value).reshape(SEQ, HA, AV)

    def attend_head(inputs_now):
        head_queries, head_keys, head_values, weight = inputs_now
        keys_wide = head_keys.astype(jnp.float32)
        values_wide = head_values.astype(jnp.float32)

        def attend_rows(query_block):
            scores = jnp.einsum('qmd,kmd->mqk', query_block.astype(jnp.float32), keys_wide, precision=HIGHEST)
            weights_raw = jnp.exp(scores - lax.optimization_barrier(jnp.max(scores, axis=-1, keepdims=True)))
            totals = lax.optimization_barrier(jnp.sum(weights_raw, axis=-1))
            rounded = lax.optimization_barrier(weights_raw.astype(jnp.bfloat16)).astype(jnp.float32)
            summed = jnp.einsum('mqk,kv->mqv', rounded, values_wide, precision=HIGHEST)
            return summed[0] / totals[0][:, None] - weight * summed[1] / totals[1][:, None]
        blocks = head_queries.reshape(SEQ // TOK_DEV, TOK_DEV, 2, AK)
        return lax.map(attend_rows, blocks).reshape(SEQ, AV)
    mixed_heads = lax.map(attend_head, (jnp.moveaxis(att_queries, 1, 0), jnp.moveaxis(att_keys, 1, 0), jnp.moveaxis(att_values, 1, 0), lambdas))
    att_rows = rms_scale(mixed_heads, att_gain).transpose(1, 0, 2).reshape(SEQ, HA * AV).astype(jnp.bfloat16)
    projected = jnp.dot(rec_rows, out_rec, preferred_element_type=jnp.float32) + jnp.dot(att_rows, out_att, preferred_element_type=jnp.float32)
    return projected.astype(jnp.bfloat16)
```

```python
import functools

import jax
import jax.numpy as jnp
from jax import lax
from jax.experimental import pallas as pl
from jax.experimental.pallas import tpu as pltpu
from jax.sharding import PartitionSpec as P

HK = 128
AK = 64
BLOCK = 64
LANES = 128
EPS = 1e-06
THETA = 500000.0
HIGHEST = lax.Precision.HIGHEST
F32 = jnp.float32
BF16 = jnp.bfloat16
PAD = 16


def rms_scale(values, gain):
    return values * lax.rsqrt(jnp.mean(values * values, axis=-1, keepdims=True) + EPS) * gain


def dot_t(a, b):
    return lax.dot_general(a, b, (((1,), (1,)), ((), ())), preferred_element_type=F32)


def dot_0(a, b):
    return lax.dot_general(a, b, (((0,), (0,)), ((), ())), preferred_element_type=F32)


def mixer_kernel(
    ranks, groups, heads, tile,
    proj, cosine, sine, leak, decay, lam, rec_gain, att_gain,
    out,
    kv, rest, swap, back, state_out, state_in, cums, adds, states, rec_sum, peak, total, mixed,
    kv_send, kv_recv, swap_send, rest_recv, state_send, state_recv, back_send, back_recv,
):
    me = lax.axis_index("sp")
    slot = lax.rem(me, groups)
    mine = lax.div(me, groups)
    length = proj.shape[1]
    rows = groups * length
    width = heads * LANES
    block_count = rows // BLOCK
    partner_slot = groups - 1 - slot
    partner = mine * groups + partner_slot
    blocks = ranks // groups
    own_rows = pl.ds(pl.multiple_of(slot * length, length), length)
    other_rows = pl.ds(pl.multiple_of(partner_slot * length, length), length)

    barrier = pltpu.get_barrier_semaphore()
    peers = []
    for k in range(1, blocks):
        peers.append(lax.rem(mine + k, blocks))
    for peer in peers:
        pl.semaphore_signal(barrier, inc=1, device_id={"sp": peer * groups + slot})
    if groups > 1:
        pl.semaphore_signal(barrier, inc=1, device_id={"sp": partner})

    lane = lax.broadcasted_iota(jnp.int32, (length, LANES), 1)
    low_half = lax.rem(lane, AK) < AK // 2

    def rotated(raw):
        wide = raw.astype(F32)
        turned = jnp.where(low_half, -pltpu.roll(wide, LANES - AK // 2, 1), pltpu.roll(wide, AK // 2, 1))
        return wide * cosine[...] + turned * sine[...]

    def prepare(head_group, key_value, others):
        for h in range(heads):
            at = h * LANES
            key_value[:, at : at + LANES] = rotated(proj[head_group, :, at : at + LANES]).astype(BF16)
        key_value[:, width : 2 * width] = proj[head_group, :, width : 2 * width]
        for h in range(heads):
            at = 2 * width + h * LANES
            others[:, h * LANES : (h + 1) * LANES] = (
                rotated(proj[head_group, :, at : at + LANES]) * AK ** (-0.5)
            ).astype(BF16)
        others[:, width:] = proj[head_group, :, 3 * width :]

    if groups > 1:
        prepare(partner_slot, swap.at[:, : 2 * width], swap.at[:, 2 * width :])
    prepare(slot, kv.at[mine, own_rows], rest.at[own_rows])
    pl.semaphore_wait(barrier, blocks - 1 + (groups - 1))

    def block_copy(source_rows, source_slot, peer):
        return pltpu.make_async_remote_copy(
            src_ref=kv.at[mine, source_rows],
            dst_ref=kv.at[mine, source_rows],
            send_sem=kv_send.at[peer, source_slot],
            recv_sem=kv_recv.at[mine, source_slot],
            device_id={"sp": peer * groups + slot},
        )

    def arrival(block, piece):
        piece_rows = pl.ds(pl.multiple_of(piece * length, length), length)
        return pltpu.make_async_remote_copy(
            src_ref=kv.at[block, piece_rows],
            dst_ref=kv.at[block, piece_rows],
            send_sem=kv_send.at[block, piece],
            recv_sem=kv_recv.at[block, piece],
            device_id={"sp": block * groups + slot},
        )

    if groups > 1:
        swap_kv = pltpu.make_async_remote_copy(
            src_ref=swap.at[:, : 2 * width],
            dst_ref=kv.at[mine, own_rows],
            send_sem=swap_send.at[0],
            recv_sem=kv_recv.at[mine, slot],
            device_id={"sp": partner},
        )
        swap_kv.start()
        swap_rest = pltpu.make_async_remote_copy(
            src_ref=swap.at[:, 2 * width :],
            dst_ref=rest.at[own_rows],
            send_sem=swap_send.at[1],
            recv_sem=rest_recv,
            device_id={"sp": partner},
        )
    own_copies = [block_copy(own_rows, slot, peer) for peer in peers]
    for copy in own_copies:
        copy.start()
    other_copies = []
    if groups > 1:
        swap_rest.start()
        arrival(mine, partner_slot).wait_recv()
        other_copies = [block_copy(other_rows, partner_slot, peer) for peer in peers]
        for copy in other_copies:
            copy.start()
        swap_rest.wait_recv()

    row_at = lax.broadcasted_iota(jnp.int32, (BLOCK, BLOCK), 0)
    col_at = lax.broadcasted_iota(jnp.int32, (BLOCK, BLOCK), 1)
    earlier = (row_at >= col_at, row_at <= col_at)
    triangles = tuple(mask.astype(F32) for mask in earlier)
    ends = (BLOCK - 1, 0)
    middles = (BLOCK // 2 - 1, BLOCK // 2)

    def rows_of(direction, step):
        index = step if direction == 0 else block_count - 1 - step
        return index, pl.ds(pl.multiple_of(index * BLOCK, BLOCK), BLOCK)

    def part(at, index, h):
        return rest[at, (index * heads + h) * LANES : (index * heads + h + 1) * LANES].astype(F32)

    def keys_of(at, direction, h):
        return leak[h, direction : direction + 1, :] * jax.nn.sigmoid(-part(at, 2 + direction, h))

    states[...] = jnp.zeros_like(states)
    rec_sum[...] = jnp.zeros_like(rec_sum)

    def first_pass(step, totals):
        after = []
        for h in range(heads):
            for d in range(2):
                index, at = rows_of(d, step)
                keys = keys_of(at, d, h)
                column = d * heads + h
                logs = jnp.log1p(-keys) + decay[at, column : column + 1]
                cum = jnp.dot(triangles[d], logs, precision=HIGHEST, preferred_element_type=F32)
                cums[h, d, at, :] = cum
                last = cum[ends[d] : ends[d] + 1, :]
                scaled = (keys * jnp.exp(last - cum)).astype(BF16)
                added = dot_0(part(at, 4, h).astype(BF16), scaled)
                adds[h, d, index] = added
                states[h, d] = states[h, d] * jnp.exp(last) + added
                after.append(totals[h * 2 + d] + last)
        return tuple(after)

    nothing = tuple(jnp.zeros((1, LANES), F32) for _ in range(2 * heads))
    sums = lax.fori_loop(0, block_count, first_pass, nothing, unroll=2)
    for h in range(heads):
        for d in range(2):
            state_out[d, h, :LANES, :] = states[h, d].astype(BF16)
            factor = jnp.broadcast_to(jnp.exp(sums[h * 2 + d]), (PAD, LANES))
            coarse = factor.astype(BF16)
            fine = (factor - coarse.astype(F32)).astype(BF16)
            first_row = lax.broadcasted_iota(jnp.int32, (PAD, LANES), 0) == 0
            state_out[d, h, LANES:, :] = jnp.where(first_row, coarse.astype(F32), fine.astype(F32)).astype(BF16)
    state_copies = []
    for peer in peers:
        copy = pltpu.make_async_remote_copy(
            src_ref=state_out.at[jnp.where(peer > mine, 0, 1)],
            dst_ref=state_in.at[mine],
            send_sem=state_send.at[peer],
            recv_sem=state_recv.at[mine],
            device_id={"sp": peer * groups + slot},
        )
        copy.start()
        state_copies.append(copy)

    lane_q = lax.broadcasted_iota(jnp.int32, (tile, LANES), 1)
    tiles = rows // tile
    peak[...] = jnp.full_like(peak, -jnp.inf)
    total[...] = jnp.zeros_like(total)
    mixed[...] = jnp.zeros_like(mixed)

    def attend(block):
        for h in range(heads):
            at = h * LANES

            def one_tile(index, carry):
                q_rows = pl.ds(pl.multiple_of(index * tile, tile), tile)
                queries = rest[q_rows, at : at + LANES]
                zero = jnp.zeros_like(queries)
                both = jnp.concatenate(
                    [jnp.where(lane_q < AK, queries, zero), jnp.where(lane_q < AK, zero, queries)], axis=0
                )
                scores = dot_t(both, kv[block, :, at : at + LANES])
                before = peak[h, index][:, :1]
                raised = jnp.maximum(before, jnp.max(scores, axis=-1, keepdims=True))
                shrink = jnp.exp(before - raised)
                expo = jnp.exp(scores - raised)
                sums_now = total[h, index][:, :1] * shrink + jnp.sum(expo, axis=-1, keepdims=True)
                product = jnp.dot(
                    expo.astype(BF16), kv[block, :, width + at : width + at + LANES], preferred_element_type=F32
                )
                mixed[h, index] = mixed[h, index] * shrink + product
                peak[h, index] = jnp.broadcast_to(raised, (2 * tile, LANES))
                total[h, index] = jnp.broadcast_to(sums_now, (2 * tile, LANES))
                return carry

            lax.fori_loop(0, tiles, one_tile, 0)

    attend(mine)

    def state_arrival(block):
        return pltpu.make_async_remote_copy(
            src_ref=state_out.at[0],
            dst_ref=state_in.at[block],
            send_sem=state_send.at[block],
            recv_sem=state_recv.at[block],
            device_id={"sp": block * groups + slot},
        )

    states[...] = jnp.zeros_like(states)

    def compose(d):
        def body(step, carry):
            block = step if d == 0 else blocks - 1 - step
            state_arrival(block).wait_recv()
            for h in range(heads):
                rows_last = state_in[block, h, LANES:, :].astype(F32)
                factor = rows_last[0:1] + rows_last[1:2]
                states[h, d] = states[h, d] * factor + state_in[block, h, :LANES, :].astype(F32)
            return carry

        return body

    lax.fori_loop(0, mine, compose(0), 0)
    lax.fori_loop(0, blocks - 1 - mine, compose(1), 0)

    def second_pass(step, carry):
        for h in range(heads):
            for d in range(2):
                index, at = rows_of(d, step)
                queries = jax.nn.silu(part(at, 1, h))
                keys = keys_of(at, d, h)
                cum = cums[h, d, at, :]
                middle = cum[middles[d] : middles[d] + 1, :]
                last = cum[ends[d] : ends[d] + 1, :]
                scores = dot_t(
                    (queries * jnp.exp(cum - middle)).astype(BF16), (keys * jnp.exp(middle - cum)).astype(BF16)
                )
                scores = jnp.where(earlier[d], scores, 0.0)
                within = jnp.dot(scores.astype(BF16), part(at, 4, h).astype(BF16), preferred_element_type=F32)
                before = states[h, d]
                carried = dot_t_state(queries * jnp.exp(cum), before)
                span = slice(h * LANES, (h + 1) * LANES)
                rec_sum[at, span] = rec_sum[at, span] + within + carried
                states[h, d] = before * jnp.exp(last) + adds[h, d, index]
        return carry

    def dot_t_state(reads, state):
        return dot_t(reads.astype(BF16), state.astype(BF16))

    lax.fori_loop(0, block_count, second_pass, 0, unroll=2)

    for h in range(heads):
        span = slice(h * LANES, (h + 1) * LANES)
        out[slot, :, span] = rms_scale(rec_sum[own_rows, span], rec_gain[...]).astype(BF16)
        if groups > 1:
            back[:, span] = rms_scale(rec_sum[other_rows, span], rec_gain[...]).astype(BF16)

    def back_copy(which):
        columns = slice(which * width, (which + 1) * width)
        return pltpu.make_async_remote_copy(
            src_ref=back.at[:, columns],
            dst_ref=out.at[slot, :, columns],
            send_sem=back_send.at[which],
            recv_sem=back_recv.at[which],
            device_id={"sp": partner},
        )

    if groups > 1:
        back_copy(0).start()

    def next_block(turn, carry):
        near = lax.div(turn + 1, 2)
        away = jnp.where(lax.rem(turn, 2) == 1, near, blocks - near)
        block = lax.rem(mine + away, blocks)
        for piece in range(groups):
            arrival(block, piece).wait_recv()
        attend(block)
        return carry

    lax.fori_loop(1, blocks, next_block, 0)

    def finish(first_row, count, store):
        for h in range(heads):
            span = slice(width + h * LANES, width + (h + 1) * LANES)
            for t in range(count):
                index = first_row + t
                ratio = mixed[h, index] / total[h, index][:, :1]
                values = ratio[:tile] - lam[h] * ratio[tile:]
                store(slice(t * tile, (t + 1) * tile), span, rms_scale(values, att_gain[...]).astype(BF16))

    part_tiles = length // tile
    if groups > 1:
        def store_back(at, span, value):
            back[at, span] = value

        finish(partner_slot * part_tiles, part_tiles, store_back)
        back_copy(1).start()

    def store_own(at, span, value):
        out[slot, at, span] = value

    finish(slot * part_tiles, part_tiles, store_own)

    for copy in own_copies + other_copies + state_copies:
        copy.wait_send()
    if groups > 1:
        swap_kv.wait_send()
        swap_rest.wait_send()
        for which in range(2):
            back_copy(which).wait()


def on_device(
    tokens, norm_gain, rec_query, fwd_gate, bwd_gate, rec_value, gate_leak, log_decay, rec_gain,
    att_query, att_key, att_value, lambdas, att_gain, out_rec, out_att,
):
    ranks = lax.axis_size("sp")
    tp = lax.axis_size("tp")
    local_heads = rec_query.shape[1] // HK
    groups = 2 if local_heads % 2 == 0 and ranks % 2 == 0 else 1
    heads = local_heads // groups
    width = heads * LANES
    slot = lax.axis_index("sp") % groups

    normed = rms_scale(tokens.astype(F32), norm_gain).astype(BF16)
    order = (att_key, att_value, att_query, rec_query, fwd_gate, bwd_gate, rec_value)
    gathered = lax.all_gather(normed, "tp", axis=0, tiled=True)
    length = gathered.shape[0]
    pieces = []
    for g in range(groups):
        for weight in order:
            pieces.append(weight[:, g * width : (g + 1) * width])
    joined = jnp.concatenate(pieces, axis=1)
    projected = jnp.dot(gathered, joined, preferred_element_type=F32).astype(BF16)
    group_width = len(order) * width
    projected = jnp.stack([projected[:, g * group_width : (g + 1) * group_width] for g in range(groups)])

    positions = (lax.axis_index("sp") * length + jnp.arange(length, dtype=jnp.int32)).astype(F32)
    frequency = THETA ** (-(jnp.arange(AK // 2, dtype=F32) * 2.0 / AK))
    angles = jnp.tile(positions[:, None] * frequency[None, :], (1, LANES // (AK // 2)))
    cosine, sine = jnp.cos(angles), jnp.sin(angles)

    by_head = log_decay.reshape(2, length, groups, heads).transpose(2, 1, 0, 3).reshape(groups, length, 2 * heads)
    own_decay = lax.dynamic_index_in_dim(by_head, slot, 0, keepdims=False)
    if groups > 1:
        swapped = lax.ppermute(
            lax.dynamic_index_in_dim(by_head, groups - 1 - slot, 0, keepdims=False),
            "sp",
            [(i, i + 1 - 2 * (i % 2)) for i in range(ranks)],
        )
        decay = jnp.where(
            slot == 0, jnp.concatenate([own_decay, swapped]), jnp.concatenate([swapped, own_decay])
        )
    else:
        decay = own_decay
    leak = lax.dynamic_index_in_dim(
        gate_leak.reshape(2, groups, heads, HK).transpose(1, 2, 0, 3), slot, 0, keepdims=False
    )
    lam = lax.dynamic_index_in_dim(lambdas.reshape(groups, heads), slot, 0, keepdims=False)
    lam = jnp.broadcast_to(lam[:, None, None], (heads, 1, LANES))

    blocks = ranks // groups
    rows = groups * length
    tile = min(256, length)
    vmem = pl.BlockSpec(memory_space=pltpu.VMEM)
    dma = pltpu.SemaphoreType.DMA
    mixers = pl.pallas_call(
        functools.partial(mixer_kernel, ranks, groups, heads, tile),
        out_shape=jax.ShapeDtypeStruct((groups, length, 2 * width), BF16),
        in_specs=[vmem] * 8,
        out_specs=vmem,
        scratch_shapes=[
            pltpu.VMEM((blocks, rows, 2 * width), BF16),
            pltpu.VMEM((rows, 5 * width), BF16),
            pltpu.VMEM((length, 7 * width), BF16),
            pltpu.VMEM((length, 2 * width), BF16),
            pltpu.VMEM((2, heads, LANES + PAD, LANES), BF16),
            pltpu.VMEM((blocks, heads, LANES + PAD, LANES), BF16),
            pltpu.VMEM((heads, 2, rows, LANES), F32),
            pltpu.VMEM((heads, 2, rows // BLOCK, LANES, LANES), F32),
            pltpu.VMEM((heads, 2, LANES, LANES), F32),
            pltpu.VMEM((rows, width), F32),
            pltpu.VMEM((heads, rows // tile, 2 * tile, LANES), F32),
            pltpu.VMEM((heads, rows // tile, 2 * tile, LANES), F32),
            pltpu.VMEM((heads, rows // tile, 2 * tile, LANES), F32),
            dma((blocks, groups)),
            dma((blocks, groups)),
            dma((2,)),
            dma,
            dma((blocks,)),
            dma((blocks,)),
            dma((2,)),
            dma((2,)),
        ],
        compiler_params=pltpu.CompilerParams(
            collective_id=0, has_side_effects=True, vmem_limit_bytes=56 * 1024 * 1024
        ),
        cost_estimate=pl.CostEstimate(flops=10**10, bytes_accessed=10**7, transcendentals=10**7),
    )(projected, cosine, sine, leak, decay, lam, rec_gain.reshape(1, LANES), att_gain.reshape(1, LANES))

    shares = mixers.reshape(groups, tp, length // tp, 2, heads, LANES)
    shares = lax.all_to_all(shares, "tp", split_axis=1, concat_axis=1)
    both = shares.transpose(2, 3, 1, 0, 4, 5).reshape(length // tp, 2, -1)
    result = jnp.dot(both[:, 0], out_rec, preferred_element_type=F32) + jnp.dot(
        both[:, 1], out_att, preferred_element_type=F32
    )
    return result.astype(BF16)


def solution(mesh):
    placed = (
        P(("sp", "tp"), None), P(), P(None, "tp"), P(None, "tp"), P(None, "tp"), P(None, "tp"),
        P(None, "tp"), P(None, "sp", "tp"), P(), P(None, "tp"), P(None, "tp"), P(None, "tp"),
        P("tp"), P(), P(), P(),
    )
    return jax.shard_map(
        on_device, mesh=mesh, in_specs=placed, out_specs=P(("sp", "tp"), None), check_vma=False
    )
```

```python
import functools

import jax
import jax.numpy as jnp
from jax import lax
from jax.experimental import pallas as pl
from jax.experimental.pallas import tpu as pltpu
from jax.sharding import PartitionSpec as P

HK = 128
AK = 64
BLOCK = 64
LANES = 128
EPS = 1e-06
THETA = 500000.0
HIGHEST = lax.Precision.HIGHEST
F32 = jnp.float32
BF16 = jnp.bfloat16
PAD = 16


def rms_scale(values, gain):
    return values * lax.rsqrt(jnp.mean(values * values, axis=-1, keepdims=True) + EPS) * gain


def dot_t(a, b):
    return lax.dot_general(a, b, (((1,), (1,)), ((), ())), preferred_element_type=F32)


def dot_0(a, b):
    return lax.dot_general(a, b, (((0,), (0,)), ((), ())), preferred_element_type=F32)


def gather_kernel(tp, tokens, gain, *refs):
    weights, outs = refs[:7], refs[7:14]
    held, across, along, landed = refs[14:]
    me = lax.axis_index("tp")
    core = lax.rem(me, 2)
    pair = lax.div(me, 2)
    pairs = tp // 2
    count = tokens.shape[0]
    partner = pair * 2 + 1 - core
    others = [lax.rem(pair + k, pairs) for k in range(1, pairs)]
    barrier = pltpu.get_barrier_semaphore()
    pl.semaphore_signal(barrier, inc=1, device_id={"tp": partner})
    for q in others:
        pl.semaphore_signal(barrier, inc=1, device_id={"tp": q * 2 + core})

    def rows_at(block):
        return held.at[pl.ds(pl.multiple_of(block * count, count), count)]

    def to_partner(block):
        return pltpu.make_async_remote_copy(
            src_ref=rows_at(block),
            dst_ref=rows_at(block),
            send_sem=across.at[block],
            recv_sem=landed.at[block],
            device_id={"tp": partner},
        )

    def to_pair(q):
        return pltpu.make_async_remote_copy(
            src_ref=rows_at(me),
            dst_ref=rows_at(me),
            send_sem=along.at[q],
            recv_sem=landed.at[me],
            device_id={"tp": q * 2 + core},
        )

    normed = rms_scale(tokens[...].astype(F32), gain[...]).astype(BF16)
    held[pl.ds(pl.multiple_of(me * count, count), count), :] = normed
    pl.semaphore_wait(barrier, pairs)
    for q in others:
        to_pair(q).start()
    to_partner(me).start()

    def step(k, carry):
        q = lax.rem(pair + k, pairs)
        near = q * 2 + core

        @pl.when(k > 0)
        def _():
            to_partner(near).wait_recv()
            to_partner(near).start()

        to_partner(q * 2 + 1 - core).wait_recv()
        at = pl.ds(pl.multiple_of(q * 2 * count, 2 * count), 2 * count)
        for weight, result in zip(weights, outs):
            result[at, :] = jnp.dot(held[at, :], weight[...], preferred_element_type=F32).astype(BF16)
        return carry

    lax.fori_loop(0, pairs, step, 0)
    to_partner(me).wait_send()
    for q in others:
        to_pair(q).wait_send()
        to_partner(q * 2 + core).wait_send()


def mixer_kernel(
    ranks, tp, groups, heads, tile,
    proj_k, proj_v, proj_q, proj_rq, proj_fwd, proj_bwd, proj_rv, cosine, sine, leak, decay, lam, rec_gain, att_gain,
    out,
    kv, rest, swap, stage, state_out, state_in, cums, adds, states, rec_sum, peak, total, mixed,
    kv_send, kv_recv, swap_send, rest_recv, state_send, state_recv, out_send, out_recv,
):
    me = lax.axis_index("sp")
    slot = lax.rem(me, groups)
    mine = lax.div(me, groups)
    mesh_column = lax.axis_index("tp")
    length = proj_k.shape[0]
    piece = length // tp
    rows = groups * length
    width = heads * LANES
    block_count = rows // BLOCK
    partner_slot = groups - 1 - slot
    partner = mine * groups + partner_slot
    blocks = ranks // groups
    own_rows = pl.ds(pl.multiple_of(slot * length, length), length)
    other_rows = pl.ds(pl.multiple_of(partner_slot * length, length), length)

    barrier = pltpu.get_barrier_semaphore()
    peers = []
    for k in range(1, blocks):
        peers.append(lax.rem(mine + k, blocks))
    for peer in peers:
        pl.semaphore_signal(barrier, inc=1, device_id={"sp": peer * groups + slot})
    owners = []
    for dp in range(groups):
        for dt in range(tp):
            owners.append((dp, dt, lax.rem(slot + dp, groups), lax.rem(mesh_column + dt, tp)))
    for dp, dt, p, t in owners[1:]:
        pl.semaphore_signal(barrier, inc=1, device_id={"sp": mine * groups + p, "tp": t})

    lane = lax.broadcasted_iota(jnp.int32, (length, LANES), 1)
    low_half = lax.rem(lane, AK) < AK // 2

    def rotated(raw):
        wide = raw.astype(F32)
        turned = jnp.where(low_half, -pltpu.roll(wide, LANES - AK // 2, 1), pltpu.roll(wide, AK // 2, 1))
        return wide * cosine[...] + turned * sine[...]

    def prepare(head_group, key_value, others):
        def taken(ref, h):
            return ref[:, pl.ds(pl.multiple_of((head_group * heads + h) * LANES, LANES), LANES)]

        for h in range(heads):
            at = h * LANES
            key_value[:, at : at + LANES] = rotated(taken(proj_k, h)).astype(BF16)
            key_value[:, width + at : width + at + LANES] = taken(proj_v, h)
            others[:, at : at + LANES] = (rotated(taken(proj_q, h)) * AK ** (-0.5)).astype(BF16)
            for i, ref in enumerate((proj_rq, proj_fwd, proj_bwd, proj_rv)):
                others[:, (i + 1) * width + at : (i + 1) * width + at + LANES] = taken(ref, h)

    if groups > 1:
        prepare(partner_slot, swap.at[:, : 2 * width], swap.at[:, 2 * width :])
    prepare(slot, kv.at[mine, own_rows], rest.at[own_rows])
    pl.semaphore_wait(barrier, blocks - 1 + groups * tp - 1)

    def block_copy(source_rows, source_slot, peer):
        return pltpu.make_async_remote_copy(
            src_ref=kv.at[mine, source_rows],
            dst_ref=kv.at[mine, source_rows],
            send_sem=kv_send.at[peer, source_slot],
            recv_sem=kv_recv.at[mine, source_slot],
            device_id={"sp": peer * groups + slot},
        )

    def arrival(block, piece):
        piece_rows = pl.ds(pl.multiple_of(piece * length, length), length)
        return pltpu.make_async_remote_copy(
            src_ref=kv.at[block, piece_rows],
            dst_ref=kv.at[block, piece_rows],
            send_sem=kv_send.at[block, piece],
            recv_sem=kv_recv.at[block, piece],
            device_id={"sp": block * groups + slot},
        )

    if groups > 1:
        swap_kv = pltpu.make_async_remote_copy(
            src_ref=swap.at[:, : 2 * width],
            dst_ref=kv.at[mine, own_rows],
            send_sem=swap_send.at[0],
            recv_sem=kv_recv.at[mine, slot],
            device_id={"sp": partner},
        )
        swap_kv.start()
        swap_rest = pltpu.make_async_remote_copy(
            src_ref=swap.at[:, 2 * width :],
            dst_ref=rest.at[own_rows],
            send_sem=swap_send.at[1],
            recv_sem=rest_recv,
            device_id={"sp": partner},
        )
    own_copies = [block_copy(own_rows, slot, peer) for peer in peers]
    for copy in own_copies:
        copy.start()
    other_copies = []
    if groups > 1:
        swap_rest.start()
        arrival(mine, partner_slot).wait_recv()
        other_copies = [block_copy(other_rows, partner_slot, peer) for peer in peers]
        for copy in other_copies:
            copy.start()
        swap_rest.wait_recv()

    row_at = lax.broadcasted_iota(jnp.int32, (BLOCK, BLOCK), 0)
    col_at = lax.broadcasted_iota(jnp.int32, (BLOCK, BLOCK), 1)
    earlier = (row_at >= col_at, row_at <= col_at)
    triangles = tuple(mask.astype(F32) for mask in earlier)
    ends = (BLOCK - 1, 0)
    middles = (BLOCK // 2 - 1, BLOCK // 2)

    def rows_of(direction, step):
        index = step if direction == 0 else block_count - 1 - step
        return index, pl.ds(pl.multiple_of(index * BLOCK, BLOCK), BLOCK)

    def part(at, index, h):
        return rest[at, (index * heads + h) * LANES : (index * heads + h + 1) * LANES].astype(F32)

    def keys_of(at, direction, h):
        return leak[h, direction : direction + 1, :] * jax.nn.sigmoid(-part(at, 2 + direction, h))

    states[...] = jnp.zeros_like(states)
    rec_sum[...] = jnp.zeros_like(rec_sum)

    def first_pass(step, totals):
        after = []
        for h in range(heads):
            for d in range(2):
                index, at = rows_of(d, step)
                keys = keys_of(at, d, h)
                column = d * heads + h
                logs = jnp.log1p(-keys) + decay[at, column : column + 1]
                cum = jnp.dot(triangles[d], logs, precision=HIGHEST, preferred_element_type=F32)
                cums[h, d, at, :] = cum
                last = cum[ends[d] : ends[d] + 1, :]
                scaled = (keys * jnp.exp(last - cum)).astype(BF16)
                added = dot_0(part(at, 4, h).astype(BF16), scaled)
                adds[h, d, index] = added
                states[h, d] = states[h, d] * jnp.exp(last) + added
                after.append(totals[h * 2 + d] + last)
        return tuple(after)

    nothing = tuple(jnp.zeros((1, LANES), F32) for _ in range(2 * heads))
    sums = lax.fori_loop(0, block_count, first_pass, nothing, unroll=2)
    for h in range(heads):
        for d in range(2):
            state_out[d, h, :LANES, :] = states[h, d].astype(BF16)
            factor = jnp.broadcast_to(jnp.exp(sums[h * 2 + d]), (PAD, LANES))
            coarse = factor.astype(BF16)
            fine = (factor - coarse.astype(F32)).astype(BF16)
            first_row = lax.broadcasted_iota(jnp.int32, (PAD, LANES), 0) == 0
            state_out[d, h, LANES:, :] = jnp.where(first_row, coarse.astype(F32), fine.astype(F32)).astype(BF16)
    state_copies = []
    for peer in peers:
        copy = pltpu.make_async_remote_copy(
            src_ref=state_out.at[jnp.where(peer > mine, 0, 1)],
            dst_ref=state_in.at[mine],
            send_sem=state_send.at[peer],
            recv_sem=state_recv.at[mine],
            device_id={"sp": peer * groups + slot},
        )
        copy.start()
        state_copies.append(copy)

    lane_q = lax.broadcasted_iota(jnp.int32, (tile, LANES), 1)
    tiles = rows // tile
    peak[...] = jnp.full_like(peak, -jnp.inf)
    total[...] = jnp.zeros_like(total)
    mixed[...] = jnp.zeros_like(mixed)

    def attend(block):
        for h in range(heads):
            at = h * LANES

            def one_tile(index, carry):
                q_rows = pl.ds(pl.multiple_of(index * tile, tile), tile)
                queries = rest[q_rows, at : at + LANES]
                zero = jnp.zeros_like(queries)
                both = jnp.concatenate(
                    [jnp.where(lane_q < AK, queries, zero), jnp.where(lane_q < AK, zero, queries)], axis=0
                )
                scores = dot_t(both, kv[block, :, at : at + LANES])
                before = peak[h, index][:, :1]
                raised = jnp.maximum(before, jnp.max(scores, axis=-1, keepdims=True))
                shrink = jnp.exp(before - raised)
                expo = jnp.exp(scores - raised)
                sums_now = total[h, index][:, :1] * shrink + jnp.sum(expo, axis=-1, keepdims=True)
                product = jnp.dot(
                    expo.astype(BF16), kv[block, :, width + at : width + at + LANES], preferred_element_type=F32
                )
                mixed[h, index] = mixed[h, index] * shrink + product
                peak[h, index] = jnp.broadcast_to(raised, (2 * tile, LANES))
                total[h, index] = jnp.broadcast_to(sums_now, (2 * tile, LANES))
                return carry

            lax.fori_loop(0, tiles, one_tile, 0)

    attend(mine)

    def state_arrival(block):
        return pltpu.make_async_remote_copy(
            src_ref=state_out.at[0],
            dst_ref=state_in.at[block],
            send_sem=state_send.at[block],
            recv_sem=state_recv.at[block],
            device_id={"sp": block * groups + slot},
        )

    states[...] = jnp.zeros_like(states)

    def compose(d):
        def body(step, carry):
            block = step if d == 0 else blocks - 1 - step
            state_arrival(block).wait_recv()
            for h in range(heads):
                rows_last = state_in[block, h, LANES:, :].astype(F32)
                factor = rows_last[0:1] + rows_last[1:2]
                states[h, d] = states[h, d] * factor + state_in[block, h, :LANES, :].astype(F32)
            return carry

        return body

    lax.fori_loop(0, mine, compose(0), 0)
    lax.fori_loop(0, blocks - 1 - mine, compose(1), 0)

    def second_pass(step, carry):
        for h in range(heads):
            for d in range(2):
                index, at = rows_of(d, step)
                queries = jax.nn.silu(part(at, 1, h))
                keys = keys_of(at, d, h)
                cum = cums[h, d, at, :]
                middle = cum[middles[d] : middles[d] + 1, :]
                last = cum[ends[d] : ends[d] + 1, :]
                scores = dot_t(
                    (queries * jnp.exp(cum - middle)).astype(BF16), (keys * jnp.exp(middle - cum)).astype(BF16)
                )
                scores = jnp.where(earlier[d], scores, 0.0)
                within = jnp.dot(scores.astype(BF16), part(at, 4, h).astype(BF16), preferred_element_type=F32)
                before = states[h, d]
                carried = dot_t_state(queries * jnp.exp(cum), before)
                span = slice(h * LANES, (h + 1) * LANES)
                rec_sum[at, span] = rec_sum[at, span] + within + carried
                states[h, d] = before * jnp.exp(last) + adds[h, d, index]
        return carry

    def dot_t_state(reads, state):
        return dot_t(reads.astype(BF16), state.astype(BF16))

    lax.fori_loop(0, block_count, second_pass, 0, unroll=2)

    for h in range(heads):
        span = slice(h * LANES, (h + 1) * LANES)
        stage[:, span] = rms_scale(rec_sum[:, span], rec_gain[...]).astype(BF16)

    def hand_over(which, owner):
        dp, dt, p, t = owner
        columns = slice(which * width, (which + 1) * width)
        source = stage.at[pl.ds(pl.multiple_of(p * length + t * piece, piece), piece), columns]
        target = out.at[mesh_column, slot, :, columns]
        if dp == 0 and dt == 0:
            return pltpu.make_async_copy(source, target, out_send.at[which, dp, dt])
        return pltpu.make_async_remote_copy(
            src_ref=source,
            dst_ref=target,
            send_sem=out_send.at[which, dp, dt],
            recv_sem=out_recv.at[which, mesh_column, slot],
            device_id={"sp": mine * groups + p, "tp": t},
        )

    def taken_over(which, owner):
        dp, dt, p, t = owner
        columns = slice(which * width, (which + 1) * width)
        target = out.at[t, p, :, columns]
        return pltpu.make_async_remote_copy(
            src_ref=target,
            dst_ref=target,
            send_sem=out_send.at[which, dp, dt],
            recv_sem=out_recv.at[which, t, p],
            device_id={"sp": mine * groups + p, "tp": t},
        )

    for owner in owners:
        hand_over(0, owner).start()

    def next_block(turn, carry):
        near = lax.div(turn + 1, 2)
        away = jnp.where(lax.rem(turn, 2) == 1, near, blocks - near)
        block = lax.rem(mine + away, blocks)
        for piece in range(groups):
            arrival(block, piece).wait_recv()
        attend(block)
        return carry

    lax.fori_loop(1, blocks, next_block, 0)

    for h in range(heads):
        span = slice(width + h * LANES, width + (h + 1) * LANES)
        for index in range(tiles):
            ratio = mixed[h, index] / total[h, index][:, :1]
            values = ratio[:tile] - lam[h] * ratio[tile:]
            stage[index * tile : (index + 1) * tile, span] = rms_scale(values, att_gain[...]).astype(BF16)
    for owner in owners:
        hand_over(1, owner).start()

    for copy in own_copies + other_copies + state_copies:
        copy.wait_send()
    if groups > 1:
        swap_kv.wait_send()
        swap_rest.wait_send()
    for which in range(2):
        hand_over(which, owners[0]).wait()
        for owner in owners[1:]:
            hand_over(which, owner).wait_send()
            taken_over(which, owner).wait_recv()


def on_device(
    tokens, norm_gain, rec_query, fwd_gate, bwd_gate, rec_value, gate_leak, log_decay, rec_gain,
    att_query, att_key, att_value, lambdas, att_gain, out_rec, out_att,
):
    ranks = lax.axis_size("sp")
    tp = lax.axis_size("tp")
    local_heads = rec_query.shape[1] // HK
    groups = 2 if local_heads % 2 == 0 and ranks % 2 == 0 else 1
    heads = local_heads // groups
    width = heads * LANES
    slot = lax.axis_index("sp") % groups

    order = (att_key, att_value, att_query, rec_query, fwd_gate, bwd_gate, rec_value)
    length = tokens.shape[0] * tp
    vmem = pl.BlockSpec(memory_space=pltpu.VMEM)
    dma = pltpu.SemaphoreType.DMA
    projected = pl.pallas_call(
        functools.partial(gather_kernel, tp),
        out_shape=[jax.ShapeDtypeStruct((length, weight.shape[1]), BF16) for weight in order],
        in_specs=[vmem] * (2 + len(order)),
        out_specs=[vmem] * len(order),
        scratch_shapes=[
            pltpu.VMEM((length, tokens.shape[1]), BF16),
            dma((tp,)),
            dma((tp // 2,)),
            dma((tp,)),
        ],
        compiler_params=pltpu.CompilerParams(
            collective_id=1, has_side_effects=True, vmem_limit_bytes=40 * 1024 * 1024
        ),
        cost_estimate=pl.CostEstimate(flops=4 * 10**9, bytes_accessed=10**7, transcendentals=0),
    )(tokens, norm_gain.reshape(1, -1), *order)

    positions = (lax.axis_index("sp") * length + jnp.arange(length, dtype=jnp.int32)).astype(F32)
    frequency = THETA ** (-(jnp.arange(AK // 2, dtype=F32) * 2.0 / AK))
    angles = jnp.tile(positions[:, None] * frequency[None, :], (1, LANES // (AK // 2)))
    cosine, sine = jnp.cos(angles), jnp.sin(angles)

    by_head = log_decay.reshape(2, length, groups, heads).transpose(2, 1, 0, 3).reshape(groups, length, 2 * heads)
    own_decay = lax.dynamic_index_in_dim(by_head, slot, 0, keepdims=False)
    if groups > 1:
        swapped = lax.ppermute(
            lax.dynamic_index_in_dim(by_head, groups - 1 - slot, 0, keepdims=False),
            "sp",
            [(i, i + 1 - 2 * (i % 2)) for i in range(ranks)],
        )
        decay = jnp.where(
            slot == 0, jnp.concatenate([own_decay, swapped]), jnp.concatenate([swapped, own_decay])
        )
    else:
        decay = own_decay
    leak = lax.dynamic_index_in_dim(
        gate_leak.reshape(2, groups, heads, HK).transpose(1, 2, 0, 3), slot, 0, keepdims=False
    )
    lam = lax.dynamic_index_in_dim(lambdas.reshape(groups, heads), slot, 0, keepdims=False)
    lam = jnp.broadcast_to(lam[:, None, None], (heads, 1, LANES))

    blocks = ranks // groups
    rows = groups * length
    tile = min(256, length)
    mixers = pl.pallas_call(
        functools.partial(mixer_kernel, ranks, tp, groups, heads, tile),
        out_shape=jax.ShapeDtypeStruct((tp, groups, length // tp, 2 * width), BF16),
        in_specs=[vmem] * 14,
        out_specs=vmem,
        scratch_shapes=[
            pltpu.VMEM((blocks, rows, 2 * width), BF16),
            pltpu.VMEM((rows, 5 * width), BF16),
            pltpu.VMEM((length, 7 * width), BF16),
            pltpu.VMEM((rows, 2 * width), BF16),
            pltpu.VMEM((2, heads, LANES + PAD, LANES), BF16),
            pltpu.VMEM((blocks, heads, LANES + PAD, LANES), BF16),
            pltpu.VMEM((heads, 2, rows, LANES), F32),
            pltpu.VMEM((heads, 2, rows // BLOCK, LANES, LANES), F32),
            pltpu.VMEM((heads, 2, LANES, LANES), F32),
            pltpu.VMEM((rows, width), F32),
            pltpu.VMEM((heads, rows // tile, 2 * tile, LANES), F32),
            pltpu.VMEM((heads, rows // tile, 2 * tile, LANES), F32),
            pltpu.VMEM((heads, rows // tile, 2 * tile, LANES), F32),
            dma((blocks, groups)),
            dma((blocks, groups)),
            dma((2,)),
            dma,
            dma((blocks,)),
            dma((blocks,)),
            dma((2, groups, tp)),
            dma((2, tp, groups)),
        ],
        compiler_params=pltpu.CompilerParams(
            collective_id=0, has_side_effects=True, vmem_limit_bytes=56 * 1024 * 1024
        ),
        cost_estimate=pl.CostEstimate(flops=10**10, bytes_accessed=10**7, transcendentals=10**7),
    )(*projected, cosine, sine, leak, decay, lam, rec_gain.reshape(1, LANES), att_gain.reshape(1, LANES))

    shares = mixers.reshape(tp, groups, length // tp, 2, heads, LANES)
    both = shares.transpose(2, 3, 0, 1, 4, 5).reshape(length // tp, 2, -1)
    result = jnp.dot(both[:, 0], out_rec, preferred_element_type=F32) + jnp.dot(
        both[:, 1], out_att, preferred_element_type=F32
    )
    return result.astype(BF16)


def solution(mesh):
    placed = (
        P(("sp", "tp"), None), P(), P(None, "tp"), P(None, "tp"), P(None, "tp"), P(None, "tp"),
        P(None, "tp"), P(None, "sp", "tp"), P(), P(None, "tp"), P(None, "tp"), P(None, "tp"),
        P("tp"), P(), P(), P(),
    )
    return jax.shard_map(
        on_device, mesh=mesh, in_specs=placed, out_specs=P(("sp", "tp"), None), check_vma=False
    )
```
